32 devices in a mesh: grp: 2 (over y), sp: 4 (over z), dp: 4 (over x, core).
Axes of the slice: x: 2, y: 2, z: 4, core: 2. Of those that a mesh axis runs over, the one named last changes fastest.
Arguments:
- gate_pre: bfloat16 [8, 1, 1024, 1024], P(('grp', 'dp'), None, 'sp'), parts along dimension 0, may hold values from -6 to 6
- value_pre: bfloat16 [8, 1, 1024, 1024], P(('grp', 'dp'), None, 'sp'), parts along dimension 0, may hold values from -6 to 6
- ln_gain: bfloat16 [1024], replicated, may hold values from 0.099609375 to 1.8984375
- ln_bias: bfloat16 [1024], replicated, may hold values from -3 to 3
- spatial: bfloat16 [8, 1024, 1024], P(None, 'dp'), may hold values from -0.1875 to 0.1875
- spatial_bias: bfloat16 [8, 1024], replicated, may hold values from 0.099609375 to 1.8984375
- out_gain: bfloat16 [1024], replicated, may hold values from 0.099609375 to 1.8984375
- w_out: bfloat16 [1024, 2048], P(None, 'dp'), may hold values from -0.1875 to 0.1875
Outputs:
- mixed_out: bfloat16 [8, 1, 1024, 2048], P(('grp', 'dp'), None, 'sp'), parts along dimension 0
The draws below stay inside these ranges and needn't reach their ends.
There are 2 independent parts, one for each index of `grp`. The reference program is written for one: setup_inputs(seed, part) draws one part's arguments, and reference() takes and returns one part's arrays. A program takes and returns all parts, laid end to end along the dimension named above; an argument that names none is the same for every part. Nothing has to cross between parts.
All inputs are finite; a program needn't handle non-finite values.
Results may differ from the reference program's by a relative error of at most 0.012.
Values may be sent and summed in bfloat16 or wider, within the bound.
A program may use at most 64 MiB of HBM per device.

```python
import jax
import jax.numpy as jnp
from jax import lax

D = 2048
D_A = 1024
HEAD_DIM = 128
SEG = 128
HEADS = 8
BATCH = 4
BLK = 1024
BLOCKS = 1


def shard_levels(own_key, dims, pieces, least, largest):
    def one(position, parts):
        heights = jax.random.uniform(jax.random.fold_in(jax.random.fold_in(own_key, 6), position), (parts,), jnp.float32, least / len(pieces), largest / len(pieces))
        return jnp.repeat(jnp.exp(heights), dims[position] // parts).reshape((-1,) + (1,) * (len(dims) - position - 1))

    loudness = one(*pieces[0])
    for cut in pieces[1:]:
        loudness = loudness * one(*cut)
    return loudness


def normal_values(key, extent, scale, limit, pieces=(), dtype=jnp.bfloat16):
    factor_of = shard_levels(key, extent, pieces, -0.22, 0.18) if pieces else 1.0
    values = jax.random.normal(key, extent, jnp.float32) * scale * factor_of
    return jnp.minimum(jnp.maximum(values, -limit), limit).astype(dtype)


def setup_inputs(seed: int = 0, part: int = 0) -> dict:
    seeds = jax.random.split(jax.random.key(seed), 9)
    part_splits = jax.random.split(jax.random.fold_in(seeds[8], part), 9)
    gate_pre = normal_values(part_splits[0], (BATCH, BLOCKS, BLK, D_A), 1.0, 6.0, ((0, 4), (2, 4)))
    value_pre = normal_values(part_splits[1], (BATCH, BLOCKS, BLK, D_A), 1.0, 6.0, ((0, 4), (2, 4)))
    ln_gain = jnp.clip(1.0 + 0.18 * jax.random.normal(seeds[2], (D_A,), jnp.float32), 0.099609375, 1.8984375).astype(jnp.bfloat16)
    ln_bias = normal_values(seeds[3], (D_A,), 0.5, 3.0)
    spatial = normal_values(seeds[4], (HEADS, BLK, BLK), BLK ** -0.5, 0.1875, ((1, 4),))
    spatial_bias = jnp.clip(1.0 + 0.18 * jax.random.normal(seeds[5], (HEADS, BLK), jnp.float32), 0.099609375, 1.8984375).astype(jnp.bfloat16)
    out_gain = jnp.clip(1.0 + 0.18 * jax.random.normal(seeds[6], (D_A,), jnp.float32), 0.099609375, 1.8984375).astype(jnp.bfloat16)
    w_out = normal_values(seeds[7], (D_A, D), D_A ** -0.5, 0.1875, ((1, 4),))
    return {"gate_pre": gate_pre, "value_pre": value_pre, "ln_gain": ln_gain, "ln_bias": ln_bias, "spatial": spatial, "spatial_bias": spatial_bias, "out_gain": out_gain, "w_out": w_out}


norm_eps = 0.01
gelu_coef = 0.7978845608028654

def gelu_tanh(inputs):
    return 0.5 * inputs * (1.0 + jnp.tanh(gelu_coef * (inputs + 0.044715 * inputs * inputs * inputs)))

def reference(gate_pre, value_pre, ln_gain, ln_bias, spatial, spatial_bias, out_gain, w_out):
    head_total = spatial.shape[0]
    segment_ids = jnp.arange(BLK) // SEG
    keep_mask = segment_ids[:, None] >= segment_ids[None, :]
    weights = jnp.where(keep_mask[None], spatial, jnp.zeros_like(spatial)).astype(jnp.float32)
    bias_table = jnp.transpose(spatial_bias.astype(jnp.float32))

    def per_sequence(operands):
        gate_seq, value_seq = operands
        block_total = value_seq.shape[0]
        length = block_total * BLK
        gate_seq = gate_seq.reshape(length, gate_seq.shape[2])
        value_seq = value_seq.reshape(length, value_seq.shape[2])
        activated = gelu_tanh(value_seq.astype(jnp.float32))
        centre = lax.optimization_barrier(jnp.mean(activated, axis=-1, keepdims=True))
        centered = activated - centre
        variance = lax.optimization_barrier(jnp.mean(centered * centered, axis=-1, keepdims=True))
        values = (centered * lax.rsqrt(variance + norm_eps) * ln_gain.astype(jnp.float32) + ln_bias.astype(jnp.float32)).astype(jnp.bfloat16)
        grouped = values.reshape(block_total, BLK, head_total, HEAD_DIM).astype(jnp.float32)
        mixed = jnp.einsum('hij,njhc->nihc', weights, grouped) + bias_table[None, :, :, None]
        mixed = mixed.reshape(length, head_total * HEAD_DIM).astype(jnp.bfloat16)
        gated = gelu_tanh(gate_seq.astype(jnp.float32)) * mixed.astype(jnp.float32)
        scale = lax.rsqrt(lax.optimization_barrier(jnp.mean(gated * gated, axis=-1, keepdims=True)) + norm_eps)
        normed = (gated * scale * out_gain.astype(jnp.float32)).astype(jnp.bfloat16)
        result = jnp.dot(normed, w_out, preferred_element_type=jnp.float32).astype(jnp.bfloat16)
        return result.reshape(block_total, BLK, result.shape[1])
    return lax.map(per_sequence, (gate_pre, value_pre))
```

```python
import functools

import jax
import jax.numpy as jnp
from jax import lax
from jax.experimental import pallas as pl
from jax.experimental.pallas import tpu as pltpu
from jax.sharding import PartitionSpec as P

HEAD_DIM = 128
SEG = 128


norm_eps = 0.01
gelu_coef = 0.7978845608028654


def gelu_tanh(inputs):
    return (
        0.5 * inputs * (1.0 + jnp.tanh(gelu_coef * (inputs + 0.044715 * inputs * inputs * inputs)))
    )


def on_device(gate_pre, value_pre, ln_gain, ln_bias, spatial, spatial_bias, out_gain, w_out):
    block_total = gate_pre.shape[1]
    share = gate_pre.shape[2]
    feature_count = gate_pre.shape[3]
    token_count = block_total * share
    gate_rows = gate_pre.reshape(token_count, feature_count)
    activated = gelu_tanh(value_pre.reshape(token_count, feature_count).astype(jnp.float32))
    centre = jnp.mean(activated, axis=-1, keepdims=True)
    centered = activated - centre
    variance = jnp.mean(centered * centered, axis=-1, keepdims=True)
    values = (
        centered * lax.rsqrt(variance + norm_eps) * ln_gain.astype(jnp.float32)
        + ln_bias.astype(jnp.float32)
    ).astype(jnp.bfloat16)
    value_cols = lax.all_to_all(values, "sp", split_axis=1, concat_axis=0, tiled=True)
    length = value_cols.shape[0]
    channels = value_cols.shape[1]
    block_len = spatial.shape[2]
    sp_count = lax.axis_size("sp")
    per_head = min(channels, HEAD_DIM)
    head_count = channels // per_head
    first_head = lax.axis_index("sp") * channels // HEAD_DIM
    own_rows = lax.dynamic_slice_in_dim(spatial, first_head, head_count, 0)
    own_bias = lax.dynamic_slice_in_dim(spatial_bias, first_head, head_count, 0)
    arranged = value_cols.reshape(sp_count, block_total, share, head_count, per_head)
    arranged = jnp.transpose(arranged, (3, 0, 2, 1, 4)).reshape(
        head_count, block_len, block_total * per_head
    )
    segment_cols = jnp.arange(block_len) // SEG
    weight_piece = lax.all_gather(own_rows, "dp", axis=1, tiled=True)
    row_count = weight_piece.shape[1]
    segment_rows = jnp.arange(row_count) // SEG
    keep_mask = segment_rows[:, None] >= segment_cols[None, :]
    masked = jnp.where(keep_mask[None], weight_piece, jnp.zeros_like(weight_piece))
    products = jnp.einsum("hij,hjm->him", masked, arranged, preferred_element_type=jnp.float32)
    bias_rows = own_bias.astype(jnp.float32)
    mixed_heads = (products + bias_rows[:, :, None]).astype(jnp.bfloat16)
    mixed_cols = mixed_heads.reshape(head_count, sp_count, share, block_total, per_head)
    mixed_cols = jnp.transpose(mixed_cols, (1, 3, 2, 0, 4)).reshape(length, channels)
    mixed_rows = lax.all_to_all(mixed_cols, "sp", split_axis=0, concat_axis=1, tiled=True)
    gated_rows = gelu_tanh(gate_rows.astype(jnp.float32)) * mixed_rows.astype(jnp.float32)
    scale = lax.rsqrt(jnp.mean(gated_rows * gated_rows, axis=-1, keepdims=True) + norm_eps)
    normed = (gated_rows * scale * out_gain.astype(jnp.float32)).astype(jnp.bfloat16)
    result = jnp.dot(
        normed, lax.all_gather(w_out, "dp", axis=1, tiled=True), preferred_element_type=jnp.float32
    ).astype(jnp.bfloat16)
    return result.reshape(1, block_total, share, result.shape[1])


MESH = pl.DeviceIdType.MESH
CHUNKS = 4
ROWS = 64
PIECE = 64
EXTRA = 1
VMEM_LIMIT = 65994752
mark = jax.named_scope


def fused_kernel(
    sp_count,
    gate_hbm, value_hbm, gain_hbm, shift_hbm, spatial, bias_hbm, out_gain_hbm, w_hbm, out,
    gate_in, value_in, gate_act, vsend, vrecv, msend, mrecv, weights, w_all, normed,
    ln_gain, ln_bias, out_gain, bias, total, squares,
    local_sem, small_sem,
    v_send, v_recv, m_send, m_recv,
    sx_send, sx_recv, sy_send, sy_recv, sc_send, sc_recv, sf_send, sf_recv, sg_send, sg_recv,
    wx_send, wx_recv, wy_send, wy_recv, wc_send, wc_recv, wf_send, wf_recv, wg_send, wg_recv,
):
    g = lax.axis_index("grp")
    s = lax.axis_index("sp")
    dp = lax.axis_index("dp")
    half = lax.rem(dp, 2)
    core_peer = dp + 1 - 2 * half
    x_peer = lax.rem(dp + 2, 4)
    y_peer = 1 - g
    share, features = value_in.shape
    heads = features // HEAD_DIM
    dp_count, share_rows, block_len = weights.shape[1:]
    cuts, w_cols = w_all.shape[3], w_all.shape[5]
    pieces = sp_count * cuts
    part_width = gate_act.shape[2]
    relayed = pieces - EXTRA
    first = s * 2

    barrier = pltpu.get_barrier_semaphore()
    for off in range(1, sp_count):
        pl.semaphore_signal(
            barrier, inc=1, device_id={"sp": lax.rem(s + off, sp_count)}, device_id_type=MESH
        )
    pl.semaphore_signal(barrier, inc=1, device_id={"dp": core_peer}, device_id_type=MESH)
    pl.semaphore_signal(barrier, inc=1, device_id={"dp": x_peer}, device_id_type=MESH)
    pl.semaphore_signal(barrier, inc=1, device_id={"grp": y_peer}, device_id_type=MESH)

    load_value = pltpu.make_async_copy(value_hbm, value_in, local_sem.at[0])
    load_value.start()
    small = []
    for at, (src, dst) in enumerate(
        ((gain_hbm, ln_gain), (shift_hbm, ln_bias), (bias_hbm, bias), (out_gain_hbm, out_gain))
    ):
        copy = pltpu.make_async_copy(src, dst, small_sem.at[at])
        copy.start()
        small.append(copy)
    load_gate = pltpu.make_async_copy(gate_hbm, gate_in, local_sem.at[1])
    load_gate.start()
    load_spatial = pltpu.make_async_copy(
        spatial.at[pl.ds(first, 2)], weights.at[:, dp], local_sem.at[2]
    )
    load_spatial.start()
    load_w = []
    for part in range(2):
        copy = pltpu.make_async_copy(
            w_hbm.at[:, part], w_all.at[dp, part], local_sem.at[8 + part]
        )
        copy.start()
        load_w.append(copy)

    def send(src, dst, ssem, rsem, where):
        return pltpu.make_async_remote_copy(
            src_ref=src, dst_ref=dst, send_sem=ssem, recv_sem=rsem,
            device_id=where, device_id_type=MESH,
        )

    def on_dp(action):
        for k in range(dp_count):
            pl.when(dp == k)(functools.partial(action, k))

    s_piece = share_rows // CHUNKS

    def s_part(ref, lead, k, c):
        cols = (k * share_rows + (c + 1) * s_piece + SEG - 1) // SEG * SEG
        return ref.at[(*lead, pl.ds(c * s_piece, s_piece), pl.ds(0, cols))]

    def sx_copy(k, c):
        return send(
            s_part(spatial, (first + g,), k, c), s_part(weights, (g, k), k, c),
            sx_send.at[c], sx_recv.at[c], {"dp": x_peer},
        )

    def relay(head, k, c, ssem, rsem, where):
        piece = s_part(weights, (head, k), k, c)
        return send(piece, piece, ssem.at[c], rsem.at[c], where)

    def sx_in(k, c):
        return relay(g, k, c, sx_send, sx_recv, {"dp": x_peer})

    def sy_copy(k, c):
        return relay(g, k, c, sy_send, sy_recv, {"grp": y_peer})

    def sf_copy(k, c):
        return relay(g, k, c, sf_send, sf_recv, {"dp": core_peer})

    def sy_in(k, c):
        return relay(1 - g, k, c, sy_send, sy_recv, {"grp": y_peer})

    def sg_copy(k, c):
        return relay(1 - g, k, c, sg_send, sg_recv, {"dp": core_peer})

    def w_piece(k, part, p):
        return w_all.at[k, part, p // cuts, p % cuts]

    def wx_copy(at):
        part, p = (g, at) if at < pieces else (1 - g, at - pieces + relayed)
        return send(
            w_hbm.at[p // cuts, part, p % cuts], w_piece(dp, part, p),
            wx_send.at[at], wx_recv.at[at], {"dp": x_peer},
        )

    with mark("load_value"):
        load_value.wait()
        for copy in small:
            copy.wait()
    gain = ln_gain[...].astype(jnp.float32).reshape(1, features)
    shift = ln_bias[...].astype(jnp.float32).reshape(1, features)

    def normalise(step):
        rows = pl.ds(pl.multiple_of(step * ROWS, ROWS), ROWS)
        activated = gelu_tanh(value_in[rows, :].astype(jnp.float32))
        centre = jnp.mean(activated, axis=-1, keepdims=True)
        centered = activated - centre
        variance = jnp.mean(centered * centered, axis=-1, keepdims=True)
        values = (centered * lax.rsqrt(variance + norm_eps) * gain + shift).astype(jnp.bfloat16)
        for h in range(heads):
            vsend[h, rows, :] = values[:, h * HEAD_DIM : (h + 1) * HEAD_DIM]

    own_rows = pl.ds(pl.multiple_of(s * share, share), share)
    vs = [[], []]

    def send_values(hh, turn, slot, start, size):
        for off in range(1, sp_count):
            there = lax.rem(s + off, sp_count)
            copy = send(
                vsend.at[there * 2 + hh, pl.ds(start, size)],
                vrecv.at[hh, pl.ds(pl.multiple_of(s * share + start, size), size)],
                v_send.at[slot, off - 1], v_recv.at[slot, off - 1], {"sp": there},
            )
            copy.start()
            vs[turn].append(copy)

    steps = share // ROWS
    with mark("norm0"):
        pl.loop(0, steps // 2)(normalise)
    with mark("barrier"):
        pl.semaphore_wait(barrier, sp_count + 2)
    send_values(g, 0, 0, 0, share // 2)

    @on_dp
    def _(k):
        for c in range(CHUNKS):
            sx_copy(k, c).start()

    sc = send(
        spatial.at[pl.ds(first, 2)], weights.at[:, dp], sc_send.at[0], sc_recv.at[0],
        {"dp": core_peer},
    )
    sc.start()
    wx = [wx_copy(at) for at in range(pieces + EXTRA)]
    for copy in wx:
        copy.start()
    with mark("norm1"):
        pl.loop(steps // 2, steps)(normalise)
    send_values(g, 0, 1, share // 2, share // 2)
    send_values(1 - g, 1, 2, 0, share)
    own_v = []
    for turn in range(2):
        hh = g if turn == 0 else 1 - g
        copy = pltpu.make_async_copy(
            vsend.at[first + hh], vrecv.at[hh, own_rows], local_sem.at[4 + turn]
        )
        copy.start()
        own_v.append(copy)

    load_gate.wait()

    with mark("gact"):

        @pl.loop(0, steps)
        def _(step):
            rows = pl.ds(pl.multiple_of(step * ROWS, ROWS), ROWS)
            active = gelu_tanh(gate_in[rows, :].astype(jnp.float32))
            for h in range(heads):
                c = h // 2 * HEAD_DIM
                gate_act[h % 2, rows, c : c + HEAD_DIM] = active[
                    :, h * HEAD_DIM : (h + 1) * HEAD_DIM
                ]

    for copy in load_w:
        copy.wait()
    wc = send(w_all.at[dp], w_all.at[dp], wc_send.at[0], wc_recv.at[0], {"dp": core_peer})
    wc.start()

    @on_dp
    def _(k):
        there = (k + 2) % dp_count
        for c in range(CHUNKS):
            with mark(f"sx{c}"):
                sx_in(there, c).wait_recv()
            sy_copy(there, c).start()
            sf_copy(there, c).start()
            if c:
                with mark(f"sy{c - 1}"):
                    sy_in(there, c - 1).wait_recv()
                sg_copy(there, c - 1).start()

    wy, wf, wg = [], [], []

    def w_in(at):
        with mark(f"wx{at}"):
            wx[at].wait_recv()
        part, p = (g, at) if at < pieces else (1 - g, at - pieces + relayed)
        piece = w_piece(x_peer, part, p)
        if at < relayed:
            copy = send(piece, piece, wy_send.at[at], wy_recv.at[at], {"grp": y_peer})
            copy.start()
            wy.append(copy)
        copy = send(piece, piece, wf_send.at[at], wf_recv.at[at], {"dp": core_peer})
        copy.start()
        wf.append(copy)

    def w_pass(at):
        with mark(f"wy{at}"):
            wy[at].wait_recv()
        piece = w_piece(x_peer, 1 - g, at)
        copy = send(piece, piece, wg_send.at[at], wg_recv.at[at], {"dp": core_peer})
        copy.start()
        wg.append(copy)

    bias_all = bias[...].astype(jnp.float32)
    head_ids = lax.broadcasted_iota(jnp.int32, bias_all.shape, 0)

    def m_copy(hh, turn, k):
        rows = pl.ds(k * share, share)
        return send(
            msend.at[hh, rows], mrecv.at[hh, s],
            m_send.at[turn, k], m_recv.at[turn, s], {"sp": k},
        )

    def mix(hh, turn):
        with mark(f"v{turn}"):
            for copy in vs[turn]:
                copy.wait_recv()
            own_v[turn].wait()
        own_bias = jnp.sum(
            jnp.where(head_ids == first + hh, bias_all, 0.0), axis=0, keepdims=True
        )
        low, high = 0, sp_count - 1
        order = []
        while low <= high:
            order += [high, low] if low < high else [low]
            low, high = low + 1, high - 1
        for there in order:
            for i in range(there * share // SEG, (there + 1) * share // SEG):
                k, r = i * SEG // share_rows, i * SEG % share_rows
                reach = (i + 1) * SEG
                term = jnp.transpose(
                    jnp.broadcast_to(own_bias[:, i * SEG : (i + 1) * SEG], (HEAD_DIM, SEG))
                )
                product = jnp.dot(
                    weights[hh, k, r : r + SEG, :reach], vrecv[hh, :reach, :],
                    preferred_element_type=jnp.float32,
                )
                msend[hh, i * SEG : (i + 1) * SEG, :] = (product + term).astype(jnp.bfloat16)
            pl.when(s != there)(lambda there=there: m_copy(hh, turn, there).start())
        copy = pltpu.make_async_copy(
            msend.at[hh, own_rows], mrecv.at[hh, s], local_sem.at[6 + turn]
        )
        copy.start()
        return copy

    def m_arrived(hh, turn):
        for off in range(1, sp_count):
            there = lax.rem(s + off, sp_count)
            send(
                msend.at[hh, own_rows], mrecv.at[hh, there],
                m_send.at[turn, there], m_recv.at[turn, there], {"sp": there},
            ).wait_recv()

    def s_arrived(copy):
        @on_dp
        def _(k):
            there = (k + 1 - 2 * (k % 2) + 2) % dp_count
            for c in range(CHUNKS):
                copy(there, c).wait_recv()

    load_spatial.wait()
    sc.wait_recv()
    w_in(0)
    with mark("sf"):
        s_arrived(sf_copy)
    with mark("mix0"):
        own_m0 = mix(g, 0)
    w_in(1)

    @on_dp
    def _(k):
        there = (k + 2) % dp_count
        with mark("sy3"):
            sy_in(there, CHUNKS - 1).wait_recv()
        sg_copy(there, CHUNKS - 1).start()

    w_in(2)
    with mark("sg"):
        s_arrived(sg_copy)
    with mark("mix1"):
        own_m1 = mix(1 - g, 1)
    w_in(3)
    w_pass(0)
    w_pass(1)
    w_in(4)
    w_pass(2)

    gain_all = out_gain[...].astype(jnp.float32).reshape(1, features)
    gain_parts = [
        jnp.concatenate(
            [gain_all[:, h * HEAD_DIM : (h + 1) * HEAD_DIM] for h in range(part, heads, 2)], axis=1
        )
        for part in range(2)
    ]

    def gate_rows(hh, turn, step):
        rows = pl.ds(pl.multiple_of(step * ROWS, ROWS), ROWS)
        own_gain = jnp.where(hh == 0, gain_parts[0], gain_parts[1])
        mixed = jnp.concatenate([mrecv[hh, c, rows, :] for c in range(sp_count)], axis=-1)
        gated = gate_act[hh, rows, :] * mixed.astype(jnp.float32)
        square = jnp.sum(gated * gated, axis=-1, keepdims=True)
        if turn == 0:
            squares[rows, :] = jnp.broadcast_to(square, (ROWS, HEAD_DIM))
        else:
            mean = (squares[rows, :] + square) / features
            squares[rows, :] = lax.rsqrt(mean + norm_eps)
        normed[hh, rows, :] = (gated * own_gain).astype(jnp.bfloat16)

    def product(hh, k):
        return jnp.dot(
            normed[hh], w_all[k, hh].reshape(part_width, w_cols),
            preferred_element_type=jnp.float32,
        )

    with mark("m0"):
        m_arrived(g, 0)
        own_m0.wait()
    with mark("gate0"):
        pl.loop(0, steps)(functools.partial(gate_rows, g, 0))
    order = [dp, core_peer, x_peer, lax.rem(core_peer + 2, 4)]
    total[0] = product(g, order[0])
    wc.wait_recv()
    total[1] = product(g, order[1])
    w_in(5)
    w_pass(3)
    w_in(6)
    w_pass(4)
    for at in range(7, pieces):
        w_in(at)
    total[2] = product(g, order[2])
    for at in range(5, relayed - 1):
        w_pass(at)
    with mark("wf"):
        for copy in wf[:pieces]:
            copy.wait_recv()
    total[3] = product(g, order[3])
    for at in range(pieces, pieces + EXTRA):
        w_in(at)
    w_pass(relayed - 1)
    with mark("m1"):
        m_arrived(1 - g, 1)
        own_m1.wait()
    with mark("gate1"):
        pl.loop(0, steps)(functools.partial(gate_rows, 1 - g, 1))

    for at, k in enumerate(order):
        if at == 3:
            with mark("wg"):
                for copy in wf[pieces:] + wg:
                    copy.wait_recv()
        summed = (total[at] + product(1 - g, k)) * squares[:, :1]
        columns = pl.ds(pl.multiple_of(k * w_cols, w_cols), w_cols)
        out[:, columns] = summed.astype(jnp.bfloat16)

    with mark("endsend"):

        @on_dp
        def _(k):
            there = (k + 2) % dp_count
            for c in range(CHUNKS):
                sx_copy(k, c).wait_send()
                for copy in (sy_copy, sf_copy, sg_copy):
                    copy(there, c).wait_send()

        for turn, hh in enumerate((g, 1 - g)):
            for off in range(1, sp_count):
                m_copy(hh, turn, lax.rem(s + off, sp_count)).wait_send()
        for copy in [sc] + wx + vs[0] + vs[1] + [wc] + wy + wf + wg:
            copy.wait_send()


def fused(mesh_shape, gate_pre, value_pre, ln_gain, ln_bias, spatial, spatial_bias, out_gain, w_out):
    share, features = gate_pre.shape[2:]
    dp_count, sp_count = mesh_shape["dp"], mesh_shape["sp"]
    heads, share_rows, block_len = spatial.shape
    w_cols = w_out.shape[1]
    width = w_cols * dp_count
    bf16 = jnp.bfloat16
    dma = pltpu.SemaphoreType.DMA
    hbm = pl.BlockSpec(memory_space=pltpu.HBM)
    part_width = features // 2
    pieces = part_width // PIECE
    link_sems = []
    for count in (
        CHUNKS, CHUNKS, 1, CHUNKS, CHUNKS,
        pieces + EXTRA, pieces - EXTRA, 1, pieces + EXTRA, pieces - EXTRA,
    ):
        link_sems += [dma((count,)), dma((count,))]
    others = sp_count - 1
    result = pl.pallas_call(
        functools.partial(fused_kernel, sp_count),
        out_shape=pltpu.VMEM((share, width), bf16),
        in_specs=[hbm] * 8,
        out_specs=pl.BlockSpec(memory_space=pltpu.VMEM),
        scratch_shapes=[
            pltpu.VMEM((share, features), bf16),
            pltpu.VMEM((share, features), bf16),
            pltpu.VMEM((2, share, part_width), jnp.float32),
            pltpu.VMEM((heads, share, HEAD_DIM), bf16),
            pltpu.VMEM((2, block_len, HEAD_DIM), bf16),
            pltpu.VMEM((2, block_len, HEAD_DIM), bf16),
            pltpu.VMEM((2, sp_count, share, HEAD_DIM), bf16),
            pltpu.VMEM((2, dp_count, share_rows, block_len), bf16),
            pltpu.VMEM((dp_count, 2, sp_count, HEAD_DIM // PIECE, PIECE, w_cols), bf16),
            pltpu.VMEM((2, share, part_width), bf16),
            pltpu.VMEM((features,), bf16),
            pltpu.VMEM((features,), bf16),
            pltpu.VMEM((features,), bf16),
            pltpu.VMEM((heads, block_len), bf16),
            pltpu.VMEM((dp_count, share, w_cols), jnp.float32),
            pltpu.VMEM((share, HEAD_DIM), jnp.float32),
            dma((10,)),
            dma((4,)),
            dma((3, others)), dma((3, others)), dma((2, sp_count)), dma((2, sp_count)),
        ] + link_sems,
        compiler_params=pltpu.CompilerParams(
            collective_id=0, has_side_effects=True, vmem_limit_bytes=VMEM_LIMIT
        ),
    )(
        gate_pre.reshape(share, features), value_pre.reshape(share, features),
        ln_gain, ln_bias, spatial, spatial_bias, out_gain,
        w_out.reshape(sp_count, 2, HEAD_DIM // PIECE, PIECE, w_cols),
    )
    return result.reshape(1, 1, share, width)


def body_for(mesh_shape):
    def body(*arrays):
        gate_pre, spatial = arrays[0], arrays[4]
        blocks, share, features = gate_pre.shape[1:]
        heads, share_rows, block_len = spatial.shape
        fits = (
            mesh_shape["grp"] == 2
            and mesh_shape["dp"] == 4
            and blocks == 1
            and features == heads * HEAD_DIM
            and heads == 2 * mesh_shape["sp"]
            and share % SEG == 0
            and share_rows % SEG == 0
        )
        if fits:
            return fused(mesh_shape, *arrays)
        return on_device(*arrays)

    return body


def solution(mesh):
    in_specs = (
        P(("grp", "dp"), None, "sp", None),
        P(("grp", "dp"), None, "sp", None),
        P(),
        P(),
        P(None, "dp", None),
        P(),
        P(),
        P(None, "dp"),
    )
    out_specs = P(("grp", "dp"), None, "sp", None)
    return jax.shard_map(
        body_for(dict(mesh.shape)), mesh=mesh, in_specs=in_specs, out_specs=out_specs, check_vma=False
    )
```
